32 devices in a mesh: sp: 8 (over z, x), tp: 4 (over y, core).
Axes of the slice: x: 2, y: 2, z: 4, core: 2. Of those that a mesh axis runs over, the one named last changes fastest.
Arguments:
- queries: bfloat16 [1024, 2048], P('sp', 'tp'), may hold values from -18 to 90
- projected_key_rows: bfloat16 [1024, 1024], P('sp', 'tp'), may hold values from -18 to 90
- projected_value_rows: bfloat16 [1024, 1024], P('sp', 'tp'), may hold values from -6 to 6
- query_gain: float32 [64], replicated, may hold values from 1 to 6
- key_norm_gain: float32 [64], replicated, may hold values from 1 to 6
- residual: bfloat16 [1024, 2048], P('sp', 'tp'), may hold values from -54 to 54
- out_weight: bfloat16 [2048, 2048], P('tp'), may hold values from -1 to 1
- norm_gain: float32 [2048], P('tp'), may hold values from 0.28 to 4.68
- expert_ids: int32 [1024, 2], P('sp'), may hold values from 0 to 7, as said below
- route_weights: float32 [1024, 2], P('sp'), may hold values from 0.2 to 1
- gate_weight: bfloat16 [8, 2048, 4096], P('sp', None, 'tp'), may hold values from -0.125 to 0.125
- up_weight: bfloat16 [8, 2048, 4096], P('sp', None, 'tp'), may hold values from -0.125 to 0.125
- down_weight: bfloat16 [8, 4096, 2048], P('sp', 'tp'), may hold values from -0.25 to 0.25
- final_gain: float32 [2048], P('tp'), may hold values from 0.1 to 1.9
Outputs:
- layer_out: bfloat16 [1024, 2048], P('sp', 'tp')
The draws below stay inside these ranges and needn't reach their ends.
Inputs may be any that keep to these rules, and one draw needn't show every extreme that they name: `expert_ids`: each row names two different experts of one group, the group of expert e being e // 4. In every aligned block of 128 rows each group is named by the same number of rows, no expert is named by more than 64 rows, one expert of every group is named by exactly 64 rows, and one expert is named by 64 rows of every block.
All inputs are finite; a program needn't handle non-finite values.
Results may differ from the reference program's by a relative error of at most 0.019.
The reference program's roundings to bfloat16 on the way count: a program that leaves them out, or rounds other values in their place, can miss the bound.
Values may be sent and summed in bfloat16 or wider, within the bound.
No kernel may reach another device: no remote copies, remote signals or barrier semaphores. Data moves between devices by JAX's collectives and lax.ppermute only.
A program may use at most 64 MiB of HBM per device.

```python
import jax
import jax.numpy as jnp
from jax import lax

D = 2048
QUERY_HEAD_COUNT = 32
KEY_VALUE_HEADS = 16
HEAD_DIM = 64
GRID_W = 64
FFE = 4096
EXP_GROUP = 4
TOPK = 2
TOK_SP = 128
SEQUENCE_TOKENS = 1024
EXPERTS = 8
CAP = 64
UNIT_BLOCKS = 4


def draw_rows_by_head(key, head_count):
    normal_part = jnp.clip(jax.random.normal(jax.random.fold_in(key, 1), (SEQUENCE_TOKENS, head_count, HEAD_DIM), jnp.float32), -6.0, 6.0)
    return normal_part.reshape(SEQUENCE_TOKENS, head_count * HEAD_DIM)


def draw_queries(key, part):
    return draw_rows_by_head(jax.random.fold_in(key, 101), QUERY_HEAD_COUNT).astype(jnp.bfloat16)


def draw_projected_key_rows(key, part):
    return draw_rows_by_head(jax.random.fold_in(key, 102), KEY_VALUE_HEADS).astype(jnp.bfloat16)


def draw_gain_row(key):
    base_gain = jax.random.uniform(jax.random.fold_in(key, 1), (HEAD_DIM,), jnp.float32, 1.0, 1.8)
    return base_gain


def draw_query_gain(key, part):
    return draw_gain_row(jax.random.fold_in(key, 103))


def draw_key_norm_gain(key, part):
    return draw_gain_row(jax.random.fold_in(key, 104))


def draw_residual(key, part):
    normal_part = jnp.clip(jax.random.normal(jax.random.fold_in(key, 105), (SEQUENCE_TOKENS, D), jnp.float32), -6.0, 6.0)
    columns = jnp.arange(D, dtype=jnp.float32) / D
    return (normal_part * 0.5 * 3.0 ** columns[None, :]).astype(jnp.bfloat16)


def draw_norm_gain(key, part):
    base_gain = jax.random.uniform(jax.random.fold_in(key, 107), (D,), jnp.float32, 0.7, 1.3)
    columns = jnp.arange(D, dtype=jnp.float32) / D
    return base_gain * 0.6 * 3.0 ** columns


def draw_expert_ids(key, part):
    block_count = SEQUENCE_TOKENS // TOK_SP
    group_count = EXPERTS // EXP_GROUP
    group_rows = TOK_SP // group_count
    mean_load = 2 * group_rows // EXP_GROUP
    hot_first = jax.random.randint(jax.random.fold_in(key, 21), (), 0, EXP_GROUP)
    lane_index = jnp.arange(EXP_GROUP, dtype=jnp.int32)
    list_index = jnp.arange(2 * group_rows, dtype=jnp.int32)

    def one_group(group_key, group_number):
        heights = jax.random.randint(group_key, (EXP_GROUP,), 0, mean_load + 1)
        peak_at = jax.random.randint(jax.random.fold_in(group_key, 1), (), 0, EXP_GROUP)
        peak_at = jnp.where(group_number == 0, hot_first, peak_at)
        heights = jnp.where(lane_index == peak_at, mean_load, heights)
        heights = jnp.where(lane_index == (peak_at + EXP_GROUP - 1) % EXP_GROUP, 0, heights)
        loads = mean_load + heights - jnp.roll(heights, 1)
        ends = jnp.cumsum(loads)
        listing = jnp.sum((ends[None, :] <= list_index[:, None]).astype(jnp.int32), 1)
        return jnp.stack([listing[:group_rows], listing[group_rows:]], 1) + group_number * EXP_GROUP

    def one_block(block_key):
        group_keys = jax.random.split(block_key, group_count)
        pairs = jax.vmap(one_group)(group_keys, jnp.arange(group_count, dtype=jnp.int32)).reshape(TOK_SP, TOPK)
        order = jax.random.permutation(jax.random.fold_in(block_key, 7), TOK_SP)
        pairs = pairs[order]
        flipped = jax.random.randint(jax.random.fold_in(block_key, 8), (TOK_SP, 1), 0, 2)
        return jnp.where(flipped == 1, pairs[:, ::-1], pairs)
    block_keys = jax.random.split(jax.random.fold_in(key, 20), block_count)
    return jax.vmap(one_block)(block_keys).reshape(SEQUENCE_TOKENS, TOPK).astype(jnp.int32)


def raised(array, own_key, source, target, shards_of, factor):
    owner, partner = [(jnp.arange(array.shape[axis_at]) // (array.shape[axis_at] // shards_of)).reshape([-1 if axis == axis_at else 1 for axis in range(array.ndim)]) for axis_at in (source, target)]
    chosen = jax.random.permutation(own_key, shards_of)[partner]
    strong = (owner == chosen) | (owner == (partner + shards_of // 2) % shards_of)
    return jnp.where(strong, factor * array, array)


def levels(stream_key, extent, cuts, low, top_value):
    gain, own = 1.0, jax.random.fold_in(stream_key, 6)
    for axis_at, shards_of in cuts:
        steps = jnp.exp(jax.random.uniform(jax.random.fold_in(own, axis_at), (shards_of,), jnp.float32, low / len(cuts), top_value / len(cuts)))
        gain = gain * jnp.repeat(steps, extent[axis_at] // shards_of).reshape([-1 if axis == axis_at else 1 for axis in range(len(extent))])
    return gain


def normal_values(own_key, shape, width, most, cuts=(), kind=jnp.bfloat16):
    array = jax.random.normal(own_key, shape, jnp.float32) * width
    if len(cuts) > 0:
        array = levels(own_key, shape, cuts, -0.22, 0.18) * array
    return jnp.clip(array, min=-most, max=most).astype(kind)


def gaussian_with(own_key, dims, deviation, bound, shards, heavy, kind=jnp.bfloat16):
    entries = deviation * jax.random.normal(own_key, dims, jnp.float32)
    if shards:
        entries = entries * levels(own_key, dims, shards, -0.22, 0.18)
    return jnp.clip(raised(entries, jax.random.fold_in(own_key, 3), *heavy), -bound, bound).astype(kind)


def setup_inputs(seed: int = 0) -> dict:
    key_of = jax.random.split(jax.random.key(seed), 15)
    queries = draw_queries(jax.random.fold_in(key_of[14], 71), 0)
    projected_key_rows = draw_projected_key_rows(jax.random.fold_in(key_of[14], 71), 0)
    projected_value_rows = normal_values(key_of[2], (SEQUENCE_TOKENS, KEY_VALUE_HEADS * HEAD_DIM), 1.0, 6.0, ((0, 8), (1, 4)))
    query_gain = draw_query_gain(jax.random.fold_in(key_of[14], 71), 0)
    key_norm_gain = draw_key_norm_gain(jax.random.fold_in(key_of[14], 71), 0)
    residual = draw_residual(jax.random.fold_in(key_of[14], 71), 0)
    out_weight = gaussian_with(key_of[6], (QUERY_HEAD_COUNT * HEAD_DIM, D), (QUERY_HEAD_COUNT * HEAD_DIM // 32) ** -0.5, 1.0, ((0, 4),), (0, 1, 4, 2.0))
    norm_gain = draw_norm_gain(jax.random.fold_in(key_of[14], 71), 0)
    expert_ids = draw_expert_ids(jax.random.fold_in(key_of[14], 71), 0)
    route_weights = jnp.clip(0.2 + 0.8 * jax.random.uniform(key_of[9], (SEQUENCE_TOKENS, TOPK), jnp.float32) ** levels(key_of[9], (SEQUENCE_TOKENS, TOPK), ((0, 8),), -0.2, 0.2), 0.2, 1.0)
    gate_weight = normal_values(key_of[10], (EXPERTS, D, FFE), D ** -0.5, 0.125, ((0, 8), (2, 4)))
    up_weight = normal_values(key_of[11], (EXPERTS, D, FFE), D ** -0.5, 0.125, ((0, 8), (2, 4)))
    down_weight = gaussian_with(key_of[12], (EXPERTS, FFE, D), (FFE // 4) ** -0.5, 0.25, ((0, 8), (1, 4)), (1, 2, 4, 2.0))
    final_gain = jnp.clip(1.0 + 0.18 * jax.random.normal(key_of[13], (D,), jnp.float32), 0.1, 1.9)
    return dict(queries=queries, projected_key_rows=projected_key_rows, projected_value_rows=projected_value_rows, query_gain=query_gain, key_norm_gain=key_norm_gain, residual=residual, out_weight=out_weight, norm_gain=norm_gain, expert_ids=expert_ids, route_weights=route_weights, gate_weight=gate_weight, up_weight=up_weight, down_weight=down_weight, final_gain=final_gain)


theta_base = 10000.0
norm_epsilon = 1e-06
residual_scale = 8.0 ** 0.25

def rope_line(halves, angles):
    pair_count = angles.shape[-1]
    first_half = halves[..., :pair_count]
    second_half = halves[..., pair_count:]
    cosine = jnp.cos(angles)[:, None, :]
    sine_part = jnp.sin(angles)[:, None, :]
    return jnp.concatenate([first_half * cosine - second_half * sine_part, first_half * sine_part + second_half * cosine], -1)

def rotary_over_grid(rows_by_head, token_positions):
    head_size = rows_by_head.shape[-1]
    frequency = theta_base ** (-jnp.arange(0, head_size // 2, 2, dtype=jnp.float32) / (head_size // 2))
    grid_row = (token_positions // GRID_W).astype(jnp.float32)
    grid_col = (token_positions % GRID_W).astype(jnp.float32)
    row_part = rope_line(rows_by_head[..., :head_size // 2], grid_row[:, None] * frequency[None, :])
    col_part = rope_line(rows_by_head[..., head_size // 2:], grid_col[:, None] * frequency[None, :])
    return jnp.concatenate([row_part, col_part], -1)

def normalize_heads(token_rows, gain_row, head_count):
    shaped = token_rows.astype(jnp.float32).reshape(token_rows.shape[0], head_count, -1)
    scaled = shaped * lax.rsqrt(lax.optimization_barrier(jnp.mean(shaped * shaped, -1, keepdims=True)) + norm_epsilon)
    return scaled * gain_row[None, None, :]

def layer_norm(stream):
    center = lax.optimization_barrier(jnp.mean(stream, -1, keepdims=True))
    spread = lax.optimization_barrier(jnp.mean(jnp.square(stream - center), -1, keepdims=True))
    return (stream - center) * lax.rsqrt(spread + norm_epsilon)

def attend_group(operands):
    head_queries, head_keys, head_values = operands
    scores = jnp.einsum('gqd,kd->gqk', head_queries.astype(jnp.float32), head_keys.astype(jnp.float32)) * HEAD_DIM ** (-0.5)
    weights = jnp.exp(scores - lax.optimization_barrier(jnp.max(scores, -1, keepdims=True)))
    row_total = lax.optimization_barrier(jnp.sum(weights, -1, keepdims=True))
    rounded = lax.optimization_barrier(weights.astype(jnp.bfloat16)).astype(jnp.float32)
    gathered = jnp.einsum('gqk,kd->gqd', rounded, head_values.astype(jnp.float32))
    return (gathered / row_total).astype(jnp.bfloat16)

def block_slots(block_ids):
    onehot = (block_ids[:, None] == jnp.arange(EXPERTS, dtype=jnp.int32)[None, :]).astype(jnp.int32)
    earlier = jnp.cumsum(onehot, 0) - onehot
    return lax.optimization_barrier(jnp.sum(earlier * onehot, 1))

def expert_rows(operands):
    token_rows, gate_mat, up_mat, down_mat = operands
    gate_sum = jnp.dot(token_rows, gate_mat, preferred_element_type=jnp.float32)
    up_sum = jnp.dot(token_rows, up_mat, preferred_element_type=jnp.float32)
    hidden = (jax.nn.silu(gate_sum) * up_sum).astype(jnp.bfloat16)
    split_hidden = hidden.reshape(hidden.shape[0], UNIT_BLOCKS, -1).astype(jnp.float32)
    split_down = down_mat.reshape(UNIT_BLOCKS, -1, down_mat.shape[-1]).astype(jnp.float32)
    partial_sums = jnp.einsum('rtf,tfd->trd', split_hidden, split_down)
    rounded = lax.optimization_barrier(partial_sums.astype(jnp.bfloat16)).astype(jnp.float32)
    return lax.optimization_barrier(jnp.sum(rounded, 0)).astype(jnp.bfloat16)

def reference(queries, projected_key_rows, projected_value_rows, query_gain, key_norm_gain, residual, out_weight, norm_gain, expert_ids, route_weights, gate_weight, up_weight, down_weight, final_gain):
    token_positions = jnp.arange(SEQUENCE_TOKENS, dtype=jnp.int32)
    queries_per_group = QUERY_HEAD_COUNT // KEY_VALUE_HEADS
    queries_after_rotation = rotary_over_grid(normalize_heads(queries, query_gain, QUERY_HEAD_COUNT), token_positions).astype(jnp.bfloat16)
    keys_after_rotation = rotary_over_grid(normalize_heads(projected_key_rows, key_norm_gain, KEY_VALUE_HEADS), token_positions).astype(jnp.bfloat16)
    grouped_query_heads = queries_after_rotation.reshape(SEQUENCE_TOKENS, KEY_VALUE_HEADS, queries_per_group, HEAD_DIM).transpose(1, 2, 0, 3)
    key_heads = keys_after_rotation.transpose(1, 0, 2)
    value_per_head = projected_value_rows.reshape(SEQUENCE_TOKENS, KEY_VALUE_HEADS, HEAD_DIM).transpose(1, 0, 2)
    attended = lax.map(attend_group, (grouped_query_heads, key_heads, value_per_head))
    attended = attended.transpose(2, 0, 1, 3).reshape(SEQUENCE_TOKENS, QUERY_HEAD_COUNT * HEAD_DIM)
    mixed_rows = jnp.dot(attended, out_weight, preferred_element_type=jnp.float32)
    pre_norm = residual_scale * residual.astype(jnp.float32) + mixed_rows
    normed = (layer_norm(pre_norm) * norm_gain[None, :]).astype(jnp.bfloat16)
    block_count = SEQUENCE_TOKENS // TOK_SP
    slots = jax.vmap(block_slots)(expert_ids.reshape(block_count, TOK_SP * TOPK)).reshape(SEQUENCE_TOKENS, TOPK)
    blocks = (jnp.arange(SEQUENCE_TOKENS, dtype=jnp.int32) // TOK_SP)[:, None]
    places = expert_ids * (block_count * CAP) + blocks * CAP + slots
    routed = jnp.zeros((EXPERTS * block_count * CAP, D), jnp.bfloat16)
    routed = routed.at[places.reshape(-1)].set(jnp.repeat(normed, TOPK, axis=0))
    expert_out = lax.map(expert_rows, (routed.reshape(EXPERTS, block_count * CAP, D), gate_weight, up_weight, down_weight))
    flat_out = expert_out.reshape(-1, D)
    combined = jnp.zeros((SEQUENCE_TOKENS, D), jnp.float32)
    for route_rank in range(TOPK):
        combined = combined + route_weights[:, route_rank:route_rank + 1] * flat_out[places[:, route_rank]].astype(jnp.float32)
    second_sum = residual_scale * normed.astype(jnp.float32) + combined
    return (layer_norm(second_sum) * final_gain[None, :]).astype(jnp.bfloat16)
```

```python
import jax
import jax.numpy as jnp
from jax import lax
from jax.sharding import PartitionSpec as P

D = 2048
HEAD_DIM = 64
GRID_W = 64
TOPK = 2
EXP_GROUP = 4


theta_base = 10000.0
norm_epsilon = 1e-06
residual_scale = 8.0**0.25
far_below = -1e30


def rope_line(halves, angles):
    pair_count = angles.shape[-1]
    first_half = halves[..., :pair_count]
    second_half = halves[..., pair_count:]
    cosine = jnp.cos(angles)[:, None, :]
    sine_part = jnp.sin(angles)[:, None, :]
    return jnp.concatenate(
        [
            first_half * cosine - second_half * sine_part,
            first_half * sine_part + second_half * cosine,
        ],
        -1,
    )


def rotary_over_grid(rows_by_head, token_positions):
    head_size = rows_by_head.shape[-1]
    frequency = theta_base ** (
        -jnp.arange(0, head_size // 2, 2, dtype=jnp.float32) / (head_size // 2)
    )
    grid_row = (token_positions // GRID_W).astype(jnp.float32)
    grid_col = (token_positions % GRID_W).astype(jnp.float32)
    row_part = rope_line(
        rows_by_head[..., : head_size // 2], grid_row[:, None] * frequency[None, :]
    )
    col_part = rope_line(
        rows_by_head[..., head_size // 2 :], grid_col[:, None] * frequency[None, :]
    )
    return jnp.concatenate([row_part, col_part], -1)


def normalize_heads(token_rows, gain_row, head_count):
    shaped = token_rows.astype(jnp.float32).reshape(token_rows.shape[0], head_count, -1)
    scaled = shaped * lax.rsqrt(jnp.mean(shaped * shaped, -1, keepdims=True) + norm_epsilon)
    return scaled * gain_row[None, None, :]


def swap(values, sp_mask, tp_mask):
    tp_size = lax.axis_size("tp")
    pairs = []
    for s in range(lax.axis_size("sp")):
        for t in range(tp_size):
            pairs.append((s * tp_size + t, (s ^ sp_mask) * tp_size + (t ^ tp_mask)))
    return lax.ppermute(values, ("sp", "tp"), pairs)


def gather_tokens(own):
    chunks = [own]
    bit = lax.axis_size("sp") // 2
    while bit:
        chunks = chunks + [swap(chunk, bit, 0) for chunk in chunks]
        bit //= 2
    return chunks


def block_of(rows, block, width):
    return lax.dynamic_slice_in_dim(rows, block * width, width, 1)


def scatter_features(partial, members):
    tp_size = lax.axis_size("tp")
    width = partial.shape[1] // tp_size
    rows = partial.shape[0] // members
    place = lax.axis_index("tp")
    core, line = place % 2, place // 2
    lines = tp_size // 2
    away = [block_of(partial, 2 * (line ^ m) + 1 - core, width) for m in range(lines)]
    kept = [block_of(partial, 2 * (line ^ m) + core, width) for m in range(lines)]
    arrived = [swap(part.astype(jnp.bfloat16), 0, 1) for part in away]
    kept = [mine.astype(jnp.float32) + other.astype(jnp.float32) for mine, other in zip(kept, arrived)]
    pieces = []
    for member in range(members):
        for m in range(lines):
            if member or m:
                piece = kept[m][member * rows : (member + 1) * rows].astype(jnp.bfloat16)
                pieces.append(swap(piece, member, 2 * m))
    total = kept[0][:rows]
    for piece in pieces:
        total = total + piece.astype(jnp.float32)
    return total


def gather_rows(own, members):
    tp_size = lax.axis_size("tp")
    place = lax.axis_index("tp")
    core, line = place % 2, place // 2
    lines = tp_size // 2
    half = jnp.stack(
        [
            jnp.concatenate(
                [swap(own, member, 2 * m) if member or m else own for member in range(members)], 0
            )
            for m in range(lines)
        ]
    )
    both = jnp.concatenate([half, swap(half, 0, 1)], 0)
    ordered = [
        lax.dynamic_index_in_dim(both, ((t % 2) ^ core) * lines + ((t // 2) ^ line), 0, False)
        for t in range(tp_size)
    ]
    return jnp.concatenate(ordered, 1)


def norm_features(feature_rows, gain_row, feature_total):
    row_sums = jnp.sum(feature_rows, 1)
    squares = jnp.sum(feature_rows * feature_rows, 1)
    row_sums, squares = lax.psum((row_sums, squares), "tp")
    center = row_sums / feature_total
    spread = squares / feature_total - center * center
    return (
        (feature_rows - center[:, None])
        * lax.rsqrt(spread + norm_epsilon)[:, None]
        * gain_row[None, :]
    )


def per_device(
    queries,
    projected_key_rows,
    projected_value_rows,
    query_gain,
    key_norm_gain,
    residual,
    out_weight,
    norm_gain,
    expert_ids,
    route_weights,
    gate_weight,
    up_weight,
    down_weight,
    final_gain,
):
    token_count = queries.shape[0]
    query_heads = queries.shape[1] // HEAD_DIM
    key_heads = projected_key_rows.shape[1] // HEAD_DIM
    queries_per_group = query_heads // key_heads
    token_positions = lax.axis_index("sp") * token_count + jnp.arange(token_count, dtype=jnp.int32)
    queries_after_rotation = rotary_over_grid(
        normalize_heads(queries, query_gain, query_heads), token_positions
    ).astype(jnp.bfloat16)
    keys_after_rotation = rotary_over_grid(
        normalize_heads(projected_key_rows, key_norm_gain, key_heads), token_positions
    ).astype(jnp.bfloat16)
    packed = jnp.concatenate(
        [keys_after_rotation, projected_value_rows.reshape(token_count, key_heads, HEAD_DIM)], -1
    ).reshape(token_count, key_heads * 2 * HEAD_DIM)
    grouped_query_heads = (
        queries_after_rotation.reshape(token_count, key_heads, queries_per_group, HEAD_DIM)
        .transpose(1, 2, 0, 3)
        .reshape(key_heads, queries_per_group * token_count, HEAD_DIM)
    )
    score_scale = HEAD_DIM ** (-0.5)
    query_total = queries_per_group * token_count
    section = jnp.concatenate(gather_tokens(packed), 0)
    running_max = jnp.full((key_heads, query_total), far_below, jnp.float32)
    opened = section.reshape(section.shape[0], key_heads, 2 * HEAD_DIM)
    scores = (
        jnp.einsum(
            "hqd,khd->hqk",
            grouped_query_heads,
            opened[:, :, :HEAD_DIM],
            preferred_element_type=jnp.float32,
        )
        * score_scale
    )
    new_peak = jnp.maximum(running_max, jnp.max(scores, -1))
    weights = jnp.exp(scores - new_peak[:, :, None])
    running_sum = jnp.sum(weights, -1)
    running_out = jnp.einsum(
        "hqk,khd->hqd",
        weights.astype(jnp.bfloat16),
        opened[:, :, HEAD_DIM:],
        preferred_element_type=jnp.float32,
    )
    running_max, running_sum, running_out = (new_peak, running_sum, running_out)
    attended = (running_out / running_sum[:, :, None]).astype(jnp.bfloat16)
    attended = (
        attended.reshape(key_heads, queries_per_group, token_count, HEAD_DIM)
        .transpose(2, 0, 1, 3)
        .reshape(token_count, query_heads * HEAD_DIM)
    )
    mixed_rows = scatter_features(
        jnp.dot(attended, out_weight, preferred_element_type=jnp.float32), 1
    )
    pre_norm = residual_scale * residual.astype(jnp.float32) + mixed_rows
    normed = norm_features(pre_norm, norm_gain, D).astype(jnp.bfloat16)
    group_count = lax.axis_size("sp") // EXP_GROUP
    group_rows = token_count // group_count
    my_group = lax.axis_index("sp") // EXP_GROUP
    my_member = lax.axis_index("sp") % EXP_GROUP
    token_group = expert_ids[:, 0] // EXP_GROUP
    order = jnp.arange(token_count, dtype=jnp.int32)
    earlier = jnp.sum(
        (
            (token_group[:, None] == token_group[None, :]) & (order[None, :] < order[:, None])
        ).astype(jnp.int32),
        1,
    )
    places = (token_group ^ my_group) * group_rows + earlier
    dispatch = places[None, :] == order[:, None]
    members = jnp.arange(EXP_GROUP, dtype=jnp.int32)
    member_weights = sum(
        jnp.where(
            (expert_ids[:, k] % EXP_GROUP)[None, :] == members[:, None], route_weights[:, k][None, :], 0.0
        )
        for k in range(TOPK)
    )
    sorted_weights = lax.dot_general(
        member_weights,
        dispatch.astype(jnp.float32),
        (((1,), (1,)), ((), ())),
        precision=lax.Precision.HIGHEST,
        preferred_element_type=jnp.float32,
    )
    dispatch = dispatch.astype(jnp.bfloat16)

    def exchange(rows, axis):
        return [
            swap(
                lax.slice_in_dim(rows, offset * group_rows, (offset + 1) * group_rows, axis=axis),
                offset * EXP_GROUP,
                0,
            )
            for offset in range(1, group_count)
        ]

    held_weights = jnp.concatenate([sorted_weights[:, :group_rows]] + exchange(sorted_weights, 1), 1)
    member_tables = [held_weights] + [swap(held_weights, m, 0) for m in range(1, EXP_GROUP)]
    row_weights = [
        lax.dynamic_index_in_dim(table, my_member, 0, False) for table in member_tables
    ]
    outgoing = jnp.dot(dispatch, normed, preferred_element_type=jnp.float32).astype(jnp.bfloat16)
    foreign = exchange(outgoing, 0)
    spans = [(outgoing[:group_rows], 0, group_rows)]
    if foreign:
        spans.append((jnp.concatenate(foreign, 0), group_rows, token_count))
    results = []
    for own, start, stop in spans:
        rows = gather_rows(own, EXP_GROUP)
        gate_sum = jnp.dot(rows, gate_weight[0], preferred_element_type=jnp.float32)
        up_sum = jnp.dot(rows, up_weight[0], preferred_element_type=jnp.float32)
        hidden = (jax.nn.silu(gate_sum) * up_sum).astype(jnp.bfloat16)
        scale = jnp.concatenate([w[start:stop] for w in row_weights])
        partial = jnp.dot(hidden, down_weight[0], preferred_element_type=jnp.float32)
        results.append(
            scatter_features(partial * scale[:, None], EXP_GROUP).astype(jnp.bfloat16)
        )
    returned = [results[0]]
    for offset in range(1, group_count):
        piece = results[1][(offset - 1) * group_rows : offset * group_rows]
        returned.append(swap(piece, offset * EXP_GROUP, 0))
    combined = lax.dot_general(
        dispatch,
        jnp.concatenate(returned, 0),
        (((0,), (0,)), ((), ())),
        preferred_element_type=jnp.float32,
    )
    second_sum = residual_scale * normed.astype(jnp.float32) + combined
    return norm_features(second_sum, final_gain, D).astype(jnp.bfloat16)


def solution(mesh):
    in_specs = (
        P("sp", "tp"),
        P("sp", "tp"),
        P("sp", "tp"),
        P(),
        P(),
        P("sp", "tp"),
        P("tp", None),
        P("tp"),
        P("sp", None),
        P("sp", None),
        P("sp", None, "tp"),
        P("sp", None, "tp"),
        P("sp", "tp", None),
        P("tp"),
    )
    out_specs = P("sp", "tp")
    return jax.shard_map(
        per_device, mesh=mesh, in_specs=in_specs, out_specs=out_specs, check_vma=False
    )
```

```python
import jax
import jax.numpy as jnp
from jax import lax
from jax.sharding import PartitionSpec as P

D = 2048
HEAD_DIM = 64
GRID_W = 64
TOPK = 2
EXP_GROUP = 4


theta_base = 10000.0
norm_epsilon = 1e-06
residual_scale = 8.0**0.25
far_below = -1e30


def rope_line(halves, angles):
    pair_count = angles.shape[-1]
    first_half = halves[..., :pair_count]
    second_half = halves[..., pair_count:]
    cosine = jnp.cos(angles)[:, None, :]
    sine_part = jnp.sin(angles)[:, None, :]
    return jnp.concatenate(
        [
            first_half * cosine - second_half * sine_part,
            first_half * sine_part + second_half * cosine,
        ],
        -1,
    )


def rotary_over_grid(rows_by_head, token_positions):
    head_size = rows_by_head.shape[-1]
    frequency = theta_base ** (
        -jnp.arange(0, head_size // 2, 2, dtype=jnp.float32) / (head_size // 2)
    )
    grid_row = lax.div(token_positions, GRID_W).astype(jnp.float32)
    grid_col = lax.rem(token_positions, GRID_W).astype(jnp.float32)
    row_part = rope_line(
        rows_by_head[..., : head_size // 2], grid_row[:, None] * frequency[None, :]
    )
    col_part = rope_line(
        rows_by_head[..., head_size // 2 :], grid_col[:, None] * frequency[None, :]
    )
    return jnp.concatenate([row_part, col_part], -1)


def normalize_heads(token_rows, gain_row, head_count):
    shaped = token_rows.astype(jnp.float32).reshape(token_rows.shape[0], head_count, -1)
    scaled = shaped * lax.rsqrt(jnp.mean(shaped * shaped, -1, keepdims=True) + norm_epsilon)
    return scaled * gain_row[None, None, :]


def swap(values, sp_mask, tp_mask):
    tp_size = lax.axis_size("tp")
    pairs = []
    for s in range(lax.axis_size("sp")):
        for t in range(tp_size):
            pairs.append((s * tp_size + t, (s ^ sp_mask) * tp_size + (t ^ tp_mask)))
    return lax.ppermute(values, ("sp", "tp"), pairs)


def gather_tokens(own):
    chunks = [own]
    bit = lax.axis_size("sp") // 2
    while bit:
        chunks = chunks + [swap(chunk, bit, 0) for chunk in chunks]
        bit //= 2
    return chunks


def block_of(rows, block, width):
    return lax.dynamic_slice_in_dim(rows, block * width, width, 1)


def scatter_features(partial, members):
    tp_size = lax.axis_size("tp")
    width = partial.shape[1] // tp_size
    rows = partial.shape[0] // members
    place = lax.axis_index("tp")
    core, line = place % 2, place // 2
    lines = tp_size // 2
    away = jnp.stack([block_of(partial, 2 * (line ^ m) + 1 - core, width) for m in range(lines)])
    kept = [block_of(partial, 2 * (line ^ m) + core, width) for m in range(lines)]
    arrived = swap(away.astype(jnp.bfloat16), 0, 1)
    kept = [mine.astype(jnp.float32) + other.astype(jnp.float32) for mine, other in zip(kept, arrived)]
    pieces = []
    for member in range(members):
        for m in range(lines):
            if member or m:
                piece = kept[m][member * rows : (member + 1) * rows].astype(jnp.bfloat16)
                pieces.append(swap(piece, member, 2 * m))
    total = kept[0][:rows]
    for piece in pieces:
        total = total + piece.astype(jnp.float32)
    return total


def gather_rows(own, members):
    tp_size = lax.axis_size("tp")
    place = lax.axis_index("tp")
    core, line = place % 2, place // 2
    lines = tp_size // 2
    half = jnp.stack(
        [
            jnp.concatenate(
                [swap(own, member, 2 * m) if member or m else own for member in range(members)], 0
            )
            for m in range(lines)
        ]
    )
    both = jnp.concatenate([half, swap(half, 0, 1)], 0)
    ordered = [
        lax.dynamic_index_in_dim(both, ((t % 2) ^ core) * lines + ((t // 2) ^ line), 0, False)
        for t in range(tp_size)
    ]
    return jnp.concatenate(ordered, 1)


def norm_features(feature_rows, gain_row, feature_total):
    row_sums = jnp.sum(feature_rows, 1)
    squares = jnp.sum(feature_rows * feature_rows, 1)
    row_sums, squares = lax.psum((row_sums, squares), "tp")
    center = row_sums / feature_total
    spread = squares / feature_total - center * center
    return (
        (feature_rows - center[:, None])
        * lax.rsqrt(spread + norm_epsilon)[:, None]
        * gain_row[None, :]
    )


def per_device(
    queries,
    projected_key_rows,
    projected_value_rows,
    query_gain,
    key_norm_gain,
    residual,
    out_weight,
    norm_gain,
    expert_ids,
    route_weights,
    gate_weight,
    up_weight,
    down_weight,
    final_gain,
):
    token_count = queries.shape[0]
    query_heads = queries.shape[1] // HEAD_DIM
    key_heads = projected_key_rows.shape[1] // HEAD_DIM
    queries_per_group = query_heads // key_heads
    token_positions = lax.axis_index("sp") * token_count + jnp.arange(token_count, dtype=jnp.int32)
    queries_after_rotation = rotary_over_grid(
        normalize_heads(queries, query_gain, query_heads), token_positions
    ).astype(jnp.bfloat16)
    keys_after_rotation = rotary_over_grid(
        normalize_heads(projected_key_rows, key_norm_gain, key_heads), token_positions
    ).astype(jnp.bfloat16)
    key_width = key_heads * HEAD_DIM
    packed = jnp.concatenate(
        [keys_after_rotation.reshape(token_count, key_width), projected_value_rows], -1
    )
    grouped_query_heads = (
        queries_after_rotation.reshape(token_count, key_heads, queries_per_group, HEAD_DIM)
        .transpose(1, 2, 0, 3)
        .reshape(key_heads, queries_per_group * token_count, HEAD_DIM)
    )
    score_scale = HEAD_DIM ** (-0.5)
    query_total = queries_per_group * token_count
    section = jnp.concatenate(gather_tokens(packed), 0)
    running_max = jnp.full((key_heads, query_total), far_below, jnp.float32)
    all_keys = section[:, :key_width].reshape(-1, key_heads, HEAD_DIM)
    all_values = section[:, key_width:].reshape(-1, key_heads, HEAD_DIM)
    scores = (
        jnp.einsum(
            "hqd,khd->hqk",
            grouped_query_heads,
            all_keys,
            preferred_element_type=jnp.float32,
        )
        * score_scale
    )
    new_peak = jnp.maximum(running_max, jnp.max(scores, -1))
    weights = jnp.exp(scores - new_peak[:, :, None])
    running_sum = jnp.sum(weights, -1)
    running_out = jnp.einsum(
        "hqk,khd->hqd",
        weights.astype(jnp.bfloat16),
        all_values,
        preferred_element_type=jnp.float32,
    )
    running_max, running_sum, running_out = (new_peak, running_sum, running_out)
    attended = (running_out / running_sum[:, :, None]).astype(jnp.bfloat16)
    attended = (
        attended.reshape(key_heads, queries_per_group, token_count, HEAD_DIM)
        .transpose(2, 0, 1, 3)
        .reshape(token_count, query_heads * HEAD_DIM)
    )
    mixed_rows = scatter_features(
        jnp.dot(attended, out_weight, preferred_element_type=jnp.float32), 1
    )
    pre_norm = residual_scale * residual.astype(jnp.float32) + mixed_rows
    normed = norm_features(pre_norm, norm_gain, D).astype(jnp.bfloat16)
    group_count = lax.axis_size("sp") // EXP_GROUP
    group_rows = token_count // group_count
    my_group = lax.axis_index("sp") // EXP_GROUP
    my_member = lax.axis_index("sp") % EXP_GROUP
    token_group = lax.div(expert_ids[:, 0], EXP_GROUP)
    order = jnp.arange(token_count, dtype=jnp.int32)
    earlier = jnp.sum(
        (
            (token_group[:, None] == token_group[None, :]) & (order[None, :] < order[:, None])
        ).astype(jnp.int32),
        1,
    )
    places = (token_group ^ my_group) * group_rows + earlier
    dispatch = places[None, :] == order[:, None]
    members = jnp.arange(EXP_GROUP, dtype=jnp.int32)
    member_weights = sum(
        jnp.where(
            lax.rem(expert_ids[:, k], EXP_GROUP)[None, :] == members[:, None], route_weights[:, k][None, :], 0.0
        )
        for k in range(TOPK)
    )
    sorted_weights = lax.dot_general(
        member_weights,
        dispatch.astype(jnp.float32),
        (((1,), (1,)), ((), ())),
        precision=lax.Precision.HIGHEST,
        preferred_element_type=jnp.float32,
    )
    dispatch = dispatch.astype(jnp.bfloat16)

    def exchange(rows, axis):
        return [
            swap(
                lax.slice_in_dim(rows, offset * group_rows, (offset + 1) * group_rows, axis=axis),
                offset * EXP_GROUP,
                0,
            )
            for offset in range(1, group_count)
        ]

    outgoing = jnp.dot(dispatch, normed, preferred_element_type=jnp.float32).astype(jnp.bfloat16)
    outgoing, sorted_weights = lax.optimization_barrier((outgoing, sorted_weights))
    foreign = exchange(outgoing, 0)
    held_weights = jnp.concatenate([sorted_weights[:, :group_rows]] + exchange(sorted_weights, 1), 1)
    own_rows = jnp.concatenate([outgoing[:group_rows]] + foreign, 0)
    held_weights, own_rows = lax.optimization_barrier((held_weights, own_rows))
    rows = gather_rows(own_rows, EXP_GROUP)
    member_tables = [held_weights] + [swap(held_weights, m, 0) for m in range(1, EXP_GROUP)]
    scale = jnp.concatenate(
        [lax.dynamic_index_in_dim(table, my_member, 0, False) for table in member_tables]
    )
    gate_sum = jnp.dot(rows, gate_weight[0], preferred_element_type=jnp.float32)
    up_sum = jnp.dot(rows, up_weight[0], preferred_element_type=jnp.float32)
    hidden = (jax.nn.silu(gate_sum) * up_sum).astype(jnp.bfloat16)
    partial = jnp.dot(hidden, down_weight[0], preferred_element_type=jnp.float32)
    summed = scatter_features(partial * scale[:, None], EXP_GROUP).astype(jnp.bfloat16)
    returned = [summed[:group_rows]] + exchange(summed, 0)
    combined = lax.dot_general(
        dispatch,
        jnp.concatenate(returned, 0),
        (((0,), (0,)), ((), ())),
        preferred_element_type=jnp.float32,
    )
    second_sum = residual_scale * normed.astype(jnp.float32) + combined
    return norm_features(second_sum, final_gain, D).astype(jnp.bfloat16)


def solution(mesh):
    in_specs = (
        P("sp", "tp"),
        P("sp", "tp"),
        P("sp", "tp"),
        P(),
        P(),
        P("sp", "tp"),
        P("tp", None),
        P("tp"),
        P("sp", None),
        P("sp", None),
        P("sp", None, "tp"),
        P("sp", None, "tp"),
        P("sp", "tp", None),
        P("tp"),
    )
    out_specs = P("sp", "tp")
    return jax.shard_map(
        per_device, mesh=mesh, in_specs=in_specs, out_specs=out_specs, check_vma=False
    )
```
